32 devices in a mesh: ep: 8 (over z, x), tp: 4 (over y, core).
Axes of the slice: x: 2, y: 2, z: 4, core: 2. Of those that a mesh axis runs over, the one named last changes fastest.
Arguments:
- tokens: bfloat16 [2048, 4096], P('ep', 'tp'), may hold values from -540 to 540
- norm_gain: float32 [4096], P('tp'), may hold values from 0.1 to 1.9
- expert_ids: int32 [2048, 2], P('ep'), may hold values from 0 to 7, all different within a row; in each aligned block of 256 rows (0 to 255, 256 to 511, ...) at most 96 rows name the same one
- expert_weights: float32 [2048, 2], P('ep'), may hold values from 0.1 to 1
- gate_weight: bfloat16 [8, 4096, 2048], P('ep', None, 'tp'), may hold values from -0.09375 to 0.09375
- up_weight: bfloat16 [8, 4096, 2048], P('ep', None, 'tp'), may hold values from -0.09375 to 0.09375
- down_weight: bfloat16 [8, 2048, 4096], P('ep', None, 'tp'), may hold values from -0.125 to 0.125
Outputs:
- mixed: bfloat16 [2048, 4096], P('ep', 'tp')
The draws below stay inside these ranges and needn't reach their ends.
Inputs may be any that keep to these rules, and one draw needn't show every extreme that they name: `expert_ids`: each row names 2 different experts. Among the rows of one index of ep, no expert is named by more than 96 rows, a bound that some block reaches.
All inputs are finite; a program needn't handle non-finite values.
Results may differ from the reference program's by a relative error of at most 0.007.
Values may be sent and summed in bfloat16 or wider, within the bound.
A program may use at most 64 MiB of HBM per device.

```python
import math
import jax
import jax.numpy as jnp
import numpy as np
from jax import lax

D = 4096
FF = 2048
TOPK = 2
TOK_DEV = 256
EXPERTS = 8
CAP = 96
TOKENS = 2048
N_EP = 8


def draw_tokens(key, part):
    key_base = jax.random.fold_in(key, 11)
    key_rows = jax.random.fold_in(key, 12)
    column = jnp.arange(D, dtype=jnp.float32) / D
    row_scale = jnp.exp(jax.random.uniform(key_rows, (TOKENS, 1), jnp.float32, 0.0, math.log(10.0)))
    base = jnp.clip(jax.random.normal(key_base, (TOKENS, D), jnp.float32), -6.0, 6.0)
    column_scale = 3.0 ** column
    return (base * column_scale[None, :] * row_scale).astype(jnp.bfloat16)


def steps_of(stream_key, dims, pieces, least, largest):
    level = 1.0
    for dim, shards_of in pieces:
        draws = jax.random.uniform(jax.random.fold_in(jax.random.fold_in(stream_key, 6), dim), (shards_of,), jnp.float32, least / len(pieces), largest / len(pieces))
        level = level * jnp.repeat(jnp.exp(draws), dims[dim] // shards_of).reshape((-1,) + (1,) * (len(dims) - 1 - dim))
    return level


def shared_out(key, own, number, rows, count, top, most, slope):
    sequence = jax.random.permutation(key, count)
    packed, usual = load_shares(count, rows * top, most, slope, True), load_shares(count, rows * top, most, slope, False)
    places = jnp.arange(count)

    def named(lengths, rotation):
        used = int((lengths > 0).sum())
        fixed = max(1, used // 4)
        shifted = fixed + (places - fixed + rotation * (used - fixed)) % max(1, count - fixed)
        return jnp.zeros((count,), jnp.int32).at[sequence[jnp.where(places < fixed, places, shifted)]].set(jnp.asarray(lengths, jnp.int32))

    lengths = jnp.where(number % 4 == 0, named(packed, number // 4), named(usual, number - number // 4 - 1))
    mixed = jax.random.permutation(jax.random.fold_in(own, 3), count)
    donor, taker = mixed[0:count // 2 * 2:2], mixed[1:count // 2 * 2:2]
    slack = jnp.minimum(lengths[donor] - 1, most - lengths[taker]) // 2
    slack = jnp.where((donor == sequence[0]) | (taker == sequence[0]) | (lengths[taker] == 0), 0, jnp.maximum(slack, 0))
    shifted = jax.random.randint(jax.random.fold_in(own, 4), (count // 2,), 0, 1 << 20) % (slack + 1)
    lengths = lengths.at[donor].add(-shifted).at[taker].add(shifted)
    labels = jnp.searchsorted(jnp.cumsum(lengths), jnp.arange(rows * top), side="right").astype(jnp.int32)
    listing = labels.reshape(top, rows).T
    listing = listing[jax.random.permutation(jax.random.fold_in(own, 1), rows)]
    rotation = jax.random.randint(jax.random.fold_in(own, 2), (rows, 1), 0, top)
    return jnp.take_along_axis(listing, (jnp.arange(top)[None, :] + rotation) % top, axis=1)


def load_shares(amount, total, limit, slope, full):
    loads = [(1 << 20) // math.isqrt(rank ** slope) + 1 for rank in range(1, amount + 1)]
    largest = limit if full else min(limit, max(-(-total // amount), total * loads[0] // sum(loads)))
    least = 1 if total - largest >= amount - 1 else 0
    counts, rest = [largest] + [least] * (amount - 1), total - largest - least * (amount - 1)
    while rest > 0:
        movable = [i for i in range(1, amount) if counts[i] < largest] or [i for i in range(1, amount) if counts[i] < limit]
        pool, budget = sum([loads[i] for i in movable]), rest
        for i in movable:
            addition = min(limit - counts[i], max(1, budget * loads[i] // pool), rest)
            counts[i] = counts[i] + addition
            rest = rest - addition
    return np.array(counts)


def bell_draw(rng, shape, width, bound, cuts=(), held_as=jnp.bfloat16):
    drawn = jax.random.normal(rng, shape, jnp.float32) * width
    if len(cuts) > 0:
        drawn = steps_of(rng, shape, cuts, -0.22, 0.18) * drawn
    return jnp.clip(drawn, min=-bound, max=bound).astype(held_as)


def setup_inputs(seed: int = 0) -> dict:
    keys = jax.random.split(jax.random.key(seed), 8)
    tokens = draw_tokens(jax.random.fold_in(keys[7], 71), 0)
    norm_gain = jnp.clip(1.0 + 0.18 * jax.random.normal(keys[1], (D,), jnp.float32), 0.1, 1.9)
    expert_ids_keys = jax.random.split(jax.random.fold_in(keys[2], 1), TOKENS // TOK_DEV)
    expert_ids_turns = jax.random.permutation(jax.random.fold_in(keys[2], 3), TOKENS // TOK_DEV)
    expert_ids = jax.vmap(lambda own, number: shared_out(jax.random.fold_in(keys[2], 2), own, number, TOK_DEV, EXPERTS, TOPK, CAP, 2))(expert_ids_keys, expert_ids_turns).reshape((TOKENS, TOPK))
    expert_weights = jnp.clip(0.1 + 0.9 * jax.random.uniform(keys[3], (TOKENS, TOPK), jnp.float32) ** steps_of(keys[3], (TOKENS, TOPK), ((0, 8),), -0.2, 0.2), 0.1, 1.0)
    gate_weight = bell_draw(keys[4], (EXPERTS, D, FF), D ** -0.5, 0.09375, ((0, 8), (2, 4)))
    up_weight = bell_draw(keys[5], (EXPERTS, D, FF), D ** -0.5, 0.09375, ((0, 8), (2, 4)))
    down_weight = bell_draw(keys[6], (EXPERTS, FF, D), FF ** -0.5, 0.125, ((0, 8), (2, 4)))
    return dict(tokens=tokens, norm_gain=norm_gain, expert_ids=expert_ids, expert_weights=expert_weights, gate_weight=gate_weight, up_weight=up_weight, down_weight=down_weight)


def reference(tokens, norm_gain, expert_ids, expert_weights, gate_weight, up_weight, down_weight):
    tok_f32 = tokens.astype(jnp.float32)
    inv_rms = lax.rsqrt(lax.optimization_barrier(jnp.mean(tok_f32 * tok_f32, axis=1, keepdims=True)) + 1e-06)
    normed = (tok_f32 * inv_rms * norm_gain[None, :]).astype(jnp.bfloat16)
    per_block = TOK_DEV * TOPK
    flat_ids = expert_ids.reshape(-1).astype(jnp.int32)
    blocked = flat_ids.reshape(N_EP, per_block)
    onehot = (blocked[:, :, None] == jnp.arange(EXPERTS, dtype=jnp.int32)[None, None, :]).astype(jnp.int32)
    earlier = jnp.cumsum(onehot, axis=1) - onehot
    slot_idx = lax.optimization_barrier(jnp.sum(earlier * onehot, axis=2)).reshape(-1).astype(jnp.int32)
    source = (jnp.arange(TOKENS * TOPK, dtype=jnp.int32) // per_block).astype(jnp.int32)
    position = (source * CAP + slot_idx).astype(jnp.int32)
    token_idx = (jnp.arange(TOKENS * TOPK, dtype=jnp.int32) // TOPK).astype(jnp.int32)
    buffers = jnp.zeros((EXPERTS, N_EP * CAP, D), jnp.bfloat16).at[flat_ids, position].set(normed[token_idx])

    def one_expert(operands):
        rows_in, w_gate, w_up, w_down = operands
        gate_sum = jnp.dot(rows_in, w_gate, preferred_element_type=jnp.float32)
        up_sum = jnp.dot(rows_in, w_up, preferred_element_type=jnp.float32)
        hidden = (jax.nn.silu(gate_sum) * up_sum).astype(jnp.bfloat16)
        return jnp.dot(hidden, w_down, preferred_element_type=jnp.float32).astype(jnp.bfloat16)
    results = lax.map(one_expert, (buffers, gate_weight, up_weight, down_weight))
    picked = results[flat_ids, position].astype(jnp.float32).reshape(TOKENS, TOPK, D)
    mixed = lax.optimization_barrier(jnp.sum(picked * expert_weights[:, :, None], axis=1))
    return mixed.astype(jnp.bfloat16)
```

```python
import functools

import jax
import jax.numpy as jnp
from jax import lax
from jax.experimental import pallas as pl
from jax.experimental.pallas import tpu as pltpu
from jax.sharding import PartitionSpec as P

MESH = pl.DeviceIdType.MESH
F32 = jnp.float32
BF16 = jnp.bfloat16


INNER = (
    "s0", "t6", "a0", "o2", "o1", "o3", "a2", "b0", "c0", "r6", "p61", "p63", "p62", "q6", "a6",
    "b2", "c2", "d0", "e0", "f0", "a7", "b6", "c6", "d2", "r4", "p41", "p43", "p42", "q4", "e2",
    "a3", "b7", "c7", "d6", "e6", "f2", "a5", "b3", "c3", "d7", "f6", "e7", "f3", "a1", "b5",
    "c5", "d3", "e3", "a4", "b1", "f5", "c1", "d5", "f7", "e5", "f4", "b4", "c4", "d1", "e1",
    "d4", "e4", "f1",
)
OUTER = (
    "s0", "a0", "o2", "o3", "o1", "w4", "t4", "a2", "b0", "c0", "a3", "b2", "c2", "d0", "e0",
    "f0", "a5", "b3", "c3", "d2", "e2", "a4", "b5", "c5", "d3", "e3", "a7", "b4", "c4", "d5",
    "e5", "a6", "b7", "f2", "c7", "d4", "e4", "a1", "b6", "c6", "d7", "e7", "f3", "b1", "c1",
    "d6", "e6", "d1", "f7", "e1", "f5", "f6", "f1", "f4",
)

def kernel(
    n_ep, n_tp, groups, cap,
    tok, gain, ids, wts, gate_hbm, up_hbm, down_hbm,
    out,
    wg, wu, wd, squares_out, squares_in, key, weight, outgoing, rows, hid, prod, ret, acc,
    mine, raw, sums_out, far_ids, far_sums, far_key,
    w_sem, sq_send, sq_recv, d_send, d_recv, ry_send, rp_send, r_recv,
    hy_send, hp_send, h_recv, b_send, b_recv, f_send, f_recv,
):
    e = lax.axis_index("ep")
    t = lax.axis_index("tp")
    size = n_ep // groups
    block, place = e // size, e % size
    n_tok, width = tok.shape
    partner = t + 1 - 2 * (t % 2)
    pairs = n_tp // 2
    half = n_ep // 2
    relays = groups == 8
    inner = (block + 2) // 4 == 1

    loads = [
        pltpu.make_async_copy(gate_hbm.at[0], wg, w_sem.at[0]),
        pltpu.make_async_copy(up_hbm.at[0], wu, w_sem.at[1]),
        pltpu.make_async_copy(down_hbm.at[0], wd, w_sem.at[2]),
    ]

    barrier = pltpu.get_barrier_semaphore()
    for i in range(1, n_ep):
        pl.semaphore_signal(barrier, inc=1, device_id={"ep": (e + i) % n_ep}, device_id_type=MESH)
    for i in range(1, n_tp):
        pl.semaphore_signal(barrier, inc=1, device_id={"tp": (t + i) % n_tp}, device_id_type=MESH)
    for load in loads:
        load.start()

    def member(k, j):
        return (block ^ k) * size + (place + j) % size

    def far_copy(k, i):
        lane = 0 if k == 6 else 1
        src, dst = ((ids, far_ids), (tok, raw), (sums_out, far_sums))[i]
        return pltpu.make_async_remote_copy(
            src, dst.at[lane], f_send.at[i], f_recv.at[lane, i],
            device_id={"ep": member(k, 0)}, device_id_type=MESH)

    x = tok[...].astype(F32)
    part = jnp.sum(x * x, axis=1, keepdims=True)
    part = jnp.transpose(jnp.broadcast_to(part, (n_tok, 128)))[0:8]
    squares_out[...] = part
    pl.semaphore_wait(barrier, n_ep + n_tp - 2)

    def sq_copy(i, shard):
        return pltpu.make_async_remote_copy(
            squares_out, squares_in.at[shard], sq_send.at[i], sq_recv.at[shard],
            device_id={"tp": (t + i) % n_tp}, device_id_type=MESH)

    for i in range(1, n_tp):
        sq_copy(i, t).start()

    if relays:
        @pl.when(inner)
        def _():
            far_copy(6, 0).start()
            far_copy(6, 1).start()

    experts = key.shape[0]

    def named_slots(ids):
        which = lax.broadcasted_iota(jnp.int32, (experts, n_tok), 0)
        first, second = ids[0:1, :] == which, ids[1:2, :] == which
        named = jnp.where(first | second, 1.0, 0.0)
        before = lax.broadcasted_iota(jnp.int32, (n_tok, n_tok), 0) < lax.broadcasted_iota(
            jnp.int32, (n_tok, n_tok), 1)
        rank = jnp.dot(named.astype(BF16), jnp.where(before, 1.0, 0.0).astype(BF16),
                       preferred_element_type=F32)
        return first, second, jnp.where(first | second, rank, -1.0)

    first, second, slot = named_slots(ids)
    share = jnp.where(first, wts[0:1, :], 0.0) + jnp.where(second, wts[1:2, :], 0.0)
    for d in range(experts):
        key[d] = jnp.broadcast_to(slot[d:d + 1], (8, n_tok))
        weight[d] = jnp.broadcast_to(share[d:d + 1], (8, n_tok))

    def chosen(row, value):
        number = (lax.broadcasted_iota(jnp.int32, (cap // 8, 8, n_tok), 0) * 8
                  + lax.broadcasted_iota(jnp.int32, (cap // 8, 8, n_tok), 1)).astype(F32)
        return jnp.where(number == row[None], value, 0.0).reshape(cap, n_tok)

    def normalized(values, total):
        inv = lax.rsqrt(total / (width * n_tp) + 1e-06)
        inv = jnp.transpose(jnp.broadcast_to(inv[0:1], (128, n_tok)))[:, 0:1]
        return (values.astype(F32) * inv * gain[...]).astype(BF16)

    total = part
    for i in range(1, n_tp):
        other = (t + i) % n_tp
        sq_copy(i, other).wait_recv()
        total = total + squares_in[other]
    sums_out[...] = total
    mine[...] = normalized(tok[...], total)

    def dispatch(slot, d, s):
        return pltpu.make_async_remote_copy(
            outgoing.at[slot], rows.at[t, s], d_send.at[slot], d_recv.at[s],
            device_id={"ep": d}, device_id_type=MESH)

    def back(s, d):
        return pltpu.make_async_remote_copy(
            prod.at[s], ret.at[d], b_send.at[s], b_recv.at[d],
            device_id={"ep": s}, device_id_type=MESH)

    def peers(k):
        return range(1 if k == 0 else 0, size)

    def picked(row, values):
        return jnp.dot(chosen(row, 1.0).astype(BF16), values[...],
                       preferred_element_type=F32).astype(BF16)

    def span(k):
        return pl.ds((block ^ k) * size, size)

    def across(buf, k, i, shard, send, recv):
        ref = buf.at[shard, span(k)]
        return pltpu.make_async_remote_copy(
            ref, ref, send.at[i, k], recv.at[shard, k],
            device_id={"tp": (t + 2 * i) % n_tp}, device_id_type=MESH)

    def beside(buf, k, i, shard, send, recv):
        ref = buf.at[shard, span(k)]
        return pltpu.make_async_remote_copy(
            ref, ref, send.at[i, k], recv.at[shard, k],
            device_id={"tp": partner}, device_id_type=MESH)

    def spread(buf, k, ysend, psend, recv):
        for i in range(1, pairs):
            across(buf, k, i, t, ysend, recv).start()
        beside(buf, k, 0, t, psend, recv).start()

    def pass_on(buf, k, ysend, psend, recv):
        for i in range(1, pairs):
            shard = (t + n_tp - 2 * i) % n_tp
            across(buf, k, i, shard, ysend, recv).wait_recv()
            beside(buf, k, i, shard, psend, recv).start()

    def complete(buf, k, psend, recv):
        for i in range(pairs):
            shard = (partner + n_tp - 2 * i) % n_tp
            beside(buf, k, i, shard, psend, recv).wait_recv()

    row_sems, hid_sems = (ry_send, rp_send, r_recv), (hy_send, hp_send, h_recv)

    def own_slot(k, d):
        return d % half + (half if k >= groups // 2 else 0)

    def far_slot(lane, d):
        return d % half + half * (1 + lane)

    def run(program):
        relayed = [k for name, k in program if name == "r"]
        combined = [k for name, k in program if name == "f"]
        loaded = []

        def need(*which):
            for i in which:
                if i not in loaded:
                    loads[i].wait()
                    loaded.append(i)

        def stage_s(k):
            rows[t, e] = picked(key[e], mine)

        def stage_o(k):
            for j in peers(k):
                d = member(k, j)
                outgoing[own_slot(k, d)] = picked(key[d], mine)
                dispatch(own_slot(k, d), d, e).start()

        def stage_t(k):
            far_copy(k, 2).start()

        def stage_w(k):
            far_copy(k, 0).start()
            far_copy(k, 1).start()

        def stage_r(k):
            lane = 0 if k == 6 else 1
            for i in range(3):
                far_copy(k, i).wait_recv()
            far = named_slots(far_ids[lane])[2]
            for d in range(experts):
                far_key[lane, d] = jnp.broadcast_to(far[d:d + 1], (8, n_tok))
            raw[lane] = normalized(raw[lane], far_sums[lane])

        def stage_p(k):
            lane, k = (0, k - 60) if k >= 60 else (1, k - 40)
            source = member((6, 4)[lane], 0)
            for j in peers(k):
                d = member(k, j)
                outgoing[far_slot(lane, d)] = picked(far_key[lane, d], raw.at[lane])
                dispatch(far_slot(lane, d), d, source).start()

        def stage_q(k):
            lane = 0 if k == 6 else 1
            rows[t, member(k, 0)] = picked(far_key[lane, e], raw.at[lane])

        def stage_a(k):
            local = k == 0 or k in relayed
            for j in range(1 if local else 0, size):
                s = member(k, j)
                dispatch(s, s, s).wait_recv()
            spread(rows, k, *row_sems)

        def stage_b(k):
            pass_on(rows, k, *row_sems)

        def stage_c(k):
            complete(rows, k, rp_send, r_recv)
            need(0, 1)
            gate = up = None
            for shard in range(n_tp):
                part_rows = rows[shard, span(k)].reshape(size * cap, width)
                g = jnp.dot(part_rows, wg[shard * width:(shard + 1) * width, :],
                            preferred_element_type=F32)
                u = jnp.dot(part_rows, wu[shard * width:(shard + 1) * width, :],
                            preferred_element_type=F32)
                gate, up = (g, u) if gate is None else (gate + g, up + u)
            hidden = (gate / (1.0 + jnp.exp(-gate)) * up).astype(BF16)
            hid[t, span(k)] = hidden.reshape(size, cap, hidden.shape[1])
            spread(hid, k, *hid_sems)

        def stage_d(k):
            pass_on(hid, k, *hid_sems)

        def stage_e(k):
            complete(hid, k, hp_send, h_recv)
            need(2)
            units = hid.shape[3]
            made = None
            for shard in range(n_tp):
                m = jnp.dot(hid[shard, span(k)].reshape(size * cap, units),
                            wd[shard * units:(shard + 1) * units, :], preferred_element_type=F32)
                made = m if made is None else made + m
            prod[span(k)] = made.astype(BF16).reshape(size, cap, width)
            for j in peers(k):
                back(member(k, j), e).start()
            if k == 0:
                ret[e] = prod[e]

        def stage_f(k):
            for j in peers(k):
                d = member(k, j)
                back(d, d).wait_recv()
            base = (block ^ k) * size
            tables = jnp.concatenate(
                [chosen(key[base + j], weight[base + j][None]) for j in range(size)], axis=0)
            high = tables.astype(BF16)
            low = (tables - high.astype(F32)).astype(BF16)
            values = ret[span(k)].reshape(size * cap, width)
            dims = (((0,), (0,)), ((), ()))
            sums = lax.dot_general(high, values, dims, preferred_element_type=F32)
            sums = sums + lax.dot_general(low, values, dims, preferred_element_type=F32)
            if k != combined[0]:
                sums = sums + acc[...]
            if k != combined[-1]:
                acc[...] = sums
            else:
                out[...] = sums.astype(BF16)

        stages = dict(
            s=stage_s, o=stage_o, t=stage_t, w=stage_w, r=stage_r, p=stage_p, q=stage_q,
            a=stage_a, b=stage_b, c=stage_c, d=stage_d, e=stage_e, f=stage_f)
        for name, k in program:
            stages[name](k)

        for name, k in program:
            if name == "o":
                for j in peers(k):
                    d = member(k, j)
                    dispatch(own_slot(k, d), d, e).wait_send()
            if name == "p":
                lane, to = (0, k - 60) if k >= 60 else (1, k - 40)
                for j in peers(to):
                    d = member(to, j)
                    dispatch(far_slot(lane, d), d, e).wait_send()
            if name == "t":
                for i in range(3):
                    far_copy(k, i).wait_send()

    def steps(text):
        return [(item[0], int(item[1:])) for item in text]

    if relays:
        @pl.when(inner)
        def _():
            run(steps(INNER))

        @pl.when(jnp.logical_not(inner))
        def _():
            run(steps(OUTER))
    else:
        order = [("s", 0)] + [("o", k) for k in range(groups)]
        for k in range(groups):
            order += [(name, k) for name in "abcde"]
        run(order + [("f", k) for k in range(groups)])

    for i in range(1, n_tp):
        sq_copy(i, t).wait_send()
    for k in range(groups):
        for j in peers(k):
            back(member(k, j), e).wait_send()
        for buf, ysend, psend, recv in ((rows,) + row_sems, (hid,) + hid_sems):
            for i in range(pairs):
                if i > 0:
                    across(buf, k, i, t, ysend, recv).wait_send()
                beside(buf, k, i, t, psend, recv).wait_send()


def body(n_ep, n_tp, tokens, norm_gain, expert_ids, expert_weights, gate_weight, up_weight, down_weight):
    n_tok, width = tokens.shape
    experts = gate_weight.shape[0] * n_ep
    cap = 3 * n_tok * expert_ids.shape[1] // (2 * experts)
    depth, units = gate_weight.shape[1:]
    hidden = down_weight.shape[1]
    groups = next(g for g in (8, 4, 2, 1) if n_ep % g == 0)
    vmem = pl.BlockSpec(memory_space=pltpu.VMEM)
    hbm = pl.BlockSpec(memory_space=pl.ANY)
    dma = pltpu.SemaphoreType.DMA
    return pl.pallas_call(
        functools.partial(kernel, n_ep, n_tp, groups, cap),
        out_shape=jax.ShapeDtypeStruct((n_tok, width), BF16),
        in_specs=[vmem] * 4 + [hbm] * 3,
        out_specs=vmem,
        scratch_shapes=[
            pltpu.VMEM((depth, units), BF16),
            pltpu.VMEM((depth, units), BF16),
            pltpu.VMEM((hidden, width), BF16),
            pltpu.VMEM((8, n_tok), F32),
            pltpu.VMEM((n_tp, 8, n_tok), F32),
            pltpu.VMEM((experts, 8, n_tok), F32),
            pltpu.VMEM((experts, 8, n_tok), F32),
            pltpu.VMEM((2 * n_ep, cap, width), BF16),
            pltpu.VMEM((n_tp, n_ep, cap, width), BF16),
            pltpu.VMEM((n_tp, n_ep, cap, units), BF16),
            pltpu.VMEM((n_ep, cap, width), BF16),
            pltpu.VMEM((n_ep, cap, width), BF16),
            pltpu.VMEM((n_tok, width), F32),
            pltpu.VMEM((n_tok, width), BF16),
            pltpu.VMEM((2, n_tok, width), BF16),
            pltpu.VMEM((8, n_tok), F32),
            pltpu.VMEM((2, 2, n_tok), jnp.int32),
            pltpu.VMEM((2, 8, n_tok), F32),
            pltpu.VMEM((2, experts, 8, n_tok), F32),
            dma((3,)), dma((n_tp,)), dma((n_tp,)), dma((2 * n_ep,)), dma((n_ep,)),
            dma((n_tp // 2, groups)), dma((n_tp // 2, groups)), dma((n_tp, groups)),
            dma((n_tp // 2, groups)), dma((n_tp // 2, groups)), dma((n_tp, groups)),
            dma((n_ep,)), dma((n_ep,)), dma((3,)), dma((2, 3)),
        ],
        compiler_params=pltpu.CompilerParams(
            collective_id=0, has_side_effects=True, vmem_limit_bytes=60 * 1024 * 1024),
    )(tokens, norm_gain[None, :], expert_ids.T, expert_weights.T, gate_weight, up_weight, down_weight)


def solution(mesh):
    in_specs = (
        P("ep", "tp"),
        P("tp"),
        P("ep", None),
        P("ep", None),
        P("ep", None, "tp"),
        P("ep", None, "tp"),
        P("ep", None, "tp"),
    )
    fn = functools.partial(body, mesh.shape["ep"], mesh.shape["tp"])
    return jax.shard_map(fn, mesh=mesh, in_specs=in_specs, out_specs=P("ep", "tp"), check_vma=False)
```

```python
import functools

import jax
import jax.numpy as jnp
from jax import lax
from jax.experimental import pallas as pl
from jax.experimental.pallas import tpu as pltpu
from jax.sharding import PartitionSpec as P

MESH = pl.DeviceIdType.MESH
F32 = jnp.float32
BF16 = jnp.bfloat16


INNER = (
    "s0", "t6", "a0", "o2", "o1", "o3", "a2", "b0", "c0", "r6", "p61", "p63", "p62", "q6", "a6",
    "b2", "c2", "d0", "e0", "f0", "a7", "b6", "c6", "d2", "r4", "p41", "p43", "p42", "q4", "e2",
    "a3", "b7", "c7", "d6", "e6", "f2", "a5", "b3", "c3", "d7", "f6", "e7", "f3", "a1", "b5",
    "c5", "d3", "e3", "a4", "b1", "f5", "c1", "d5", "f7", "e5", "f4", "b4", "c4", "d1", "e1",
    "d4", "e4", "f1",
)
OUTER = (
    "s0", "a0", "o2", "o3", "o1", "w4", "t4", "a2", "b0", "c0", "a3", "b2", "c2", "d0", "e0",
    "f0", "a5", "b3", "c3", "d2", "e2", "a4", "b5", "c5", "d3", "e3", "a7", "b4", "c4", "d5",
    "e5", "a6", "b7", "f2", "c7", "d4", "e4", "a1", "b6", "c6", "d7", "e7", "f3", "b1", "c1",
    "d6", "e6", "d1", "f7", "e1", "f5", "f6", "f1", "f4",
)

def kernel(
    n_ep, n_tp, groups, cap,
    tok_hbm, gain, ids, wts, gate_hbm, up_hbm, down_hbm,
    out,
    wg, wu, wd, squares_out, squares_in, key, weight, outgoing, rows, hid, prod, ret, acc,
    mine, raw, sums_out, far_ids, far_sums, far_key, tok, gates, ups, mades,
    w_sem, sq_send, sq_recv, d_send, d_recv, ry_send, rp_send, r_recv,
    hy_send, hp_send, h_recv, b_send, b_recv, f_send, f_recv,
):
    e = lax.axis_index("ep")
    t = lax.axis_index("tp")
    size = n_ep // groups
    block, place = e // size, e % size
    n_tok, width = tok.shape
    partner = t + 1 - 2 * (t % 2)
    pairs = n_tp // 2
    half = n_ep // 2
    relays = groups == 8
    inner = (block + 2) // 4 == 1

    loads = [
        pltpu.make_async_copy(gate_hbm.at[0], wg, w_sem.at[0]),
        pltpu.make_async_copy(up_hbm.at[0], wu, w_sem.at[1]),
        pltpu.make_async_copy(down_hbm.at[0], wd, w_sem.at[2]),
    ]
    fetch = pltpu.make_async_copy(tok_hbm, tok, w_sem.at[3])
    fetch.start()

    barrier = pltpu.get_barrier_semaphore()
    for i in range(1, n_ep):
        pl.semaphore_signal(barrier, inc=1, device_id={"ep": (e + i) % n_ep}, device_id_type=MESH)
    for i in range(1, n_tp):
        pl.semaphore_signal(barrier, inc=1, device_id={"tp": (t + i) % n_tp}, device_id_type=MESH)
    for load in loads:
        load.start()

    def member(k, j):
        return (block ^ k) * size + (place + j) % size

    def far_copy(k, i):
        lane = 0 if k == 6 else 1
        src, dst = ((ids, far_ids), (tok, raw), (sums_out, far_sums))[i]
        return pltpu.make_async_remote_copy(
            src, dst.at[lane], f_send.at[i], f_recv.at[lane, i],
            device_id={"ep": member(k, 0)}, device_id_type=MESH)

    fetch.wait()
    x = tok[...].astype(F32)
    part = jnp.sum(x * x, axis=1, keepdims=True)
    part = jnp.transpose(jnp.broadcast_to(part, (n_tok, 128)))[0:8]
    squares_out[...] = part
    pl.semaphore_wait(barrier, n_ep + n_tp - 2)

    def sq_copy(i, shard):
        return pltpu.make_async_remote_copy(
            squares_out, squares_in.at[shard], sq_send.at[i], sq_recv.at[shard],
            device_id={"tp": (t + i) % n_tp}, device_id_type=MESH)

    for i in range(1, n_tp):
        sq_copy(i, t).start()

    if relays:
        @pl.when(inner)
        def _():
            far_copy(6, 0).start()
            far_copy(6, 1).start()

    experts = key.shape[0]

    def named_slots(ids):
        which = lax.broadcasted_iota(jnp.int32, (experts, n_tok), 0)
        first, second = ids[0:1, :] == which, ids[1:2, :] == which
        named = jnp.where(first | second, 1.0, 0.0)
        before = lax.broadcasted_iota(jnp.int32, (n_tok, n_tok), 0) < lax.broadcasted_iota(
            jnp.int32, (n_tok, n_tok), 1)
        rank = jnp.dot(named.astype(BF16), jnp.where(before, 1.0, 0.0).astype(BF16),
                       preferred_element_type=F32)
        return first, second, jnp.where(first | second, rank, -1.0)

    first, second, slot = named_slots(ids)
    share = jnp.where(first, wts[0:1, :], 0.0) + jnp.where(second, wts[1:2, :], 0.0)
    for d in range(experts):
        key[d] = jnp.broadcast_to(slot[d:d + 1], (8, n_tok))
        weight[d] = jnp.broadcast_to(share[d:d + 1], (8, n_tok))

    def chosen(row, value):
        number = (lax.broadcasted_iota(jnp.int32, (cap // 8, 8, n_tok), 0) * 8
                  + lax.broadcasted_iota(jnp.int32, (cap // 8, 8, n_tok), 1)).astype(F32)
        return jnp.where(number == row[None], value, 0.0).reshape(cap, n_tok)

    def normalized(values, total):
        inv = lax.rsqrt(total / (width * n_tp) + 1e-06)
        inv = jnp.transpose(jnp.broadcast_to(inv[0:1], (128, n_tok)))[:, 0:1]
        return (values.astype(F32) * inv * gain[...]).astype(BF16)

    total = part
    for i in range(1, n_tp):
        other = (t + i) % n_tp
        sq_copy(i, other).wait_recv()
        total = total + squares_in[other]
    sums_out[...] = total
    mine[...] = normalized(tok[...], total)

    def dispatch(slot, d, s):
        return pltpu.make_async_remote_copy(
            outgoing.at[slot], rows.at[t, s], d_send.at[slot], d_recv.at[s],
            device_id={"ep": d}, device_id_type=MESH)

    def back(s, d):
        return pltpu.make_async_remote_copy(
            prod.at[s], ret.at[d], b_send.at[s], b_recv.at[d],
            device_id={"ep": s}, device_id_type=MESH)

    def peers(k):
        return range(1 if k == 0 else 0, size)

    def picked(row, values):
        return jnp.dot(chosen(row, 1.0).astype(BF16), values[...],
                       preferred_element_type=F32).astype(BF16)

    def span(k):
        return pl.ds((block ^ k) * size, size)

    def across(buf, k, i, shard, send, recv):
        ref = buf.at[shard, span(k)]
        return pltpu.make_async_remote_copy(
            ref, ref, send.at[i, k], recv.at[shard, k],
            device_id={"tp": (t + 2 * i) % n_tp}, device_id_type=MESH)

    def beside(buf, k, i, shard, send, recv):
        ref = buf.at[shard, span(k)]
        return pltpu.make_async_remote_copy(
            ref, ref, send.at[i, k], recv.at[shard, k],
            device_id={"tp": partner}, device_id_type=MESH)

    def spread(buf, k, ysend, psend, recv):
        for i in range(1, pairs):
            across(buf, k, i, t, ysend, recv).start()
        beside(buf, k, 0, t, psend, recv).start()

    def pass_on(buf, k, ysend, psend, recv):
        for i in range(1, pairs):
            shard = (t + n_tp - 2 * i) % n_tp
            across(buf, k, i, shard, ysend, recv).wait_recv()
            beside(buf, k, i, shard, psend, recv).start()

    row_sems, hid_sems = (ry_send, rp_send, r_recv), (hy_send, hp_send, h_recv)

    def own_slot(k, d):
        return d % half + (half if k >= groups // 2 else 0)

    def far_slot(lane, d):
        return d % half + half * (1 + lane)

    def run(program):
        relayed = [k for name, k in program if name == "r"]
        combined = [k for name, k in program if name == "f"]
        loaded = []

        def need(*which):
            for i in which:
                if i not in loaded:
                    loads[i].wait()
                    loaded.append(i)

        def stage_s(k):
            rows[t, e] = picked(key[e], mine)

        def stage_o(k):
            for j in peers(k):
                d = member(k, j)
                outgoing[own_slot(k, d)] = picked(key[d], mine)
                dispatch(own_slot(k, d), d, e).start()

        def stage_t(k):
            far_copy(k, 2).start()

        def stage_w(k):
            far_copy(k, 0).start()
            far_copy(k, 1).start()

        def stage_r(k):
            lane = 0 if k == 6 else 1
            for i in range(3):
                far_copy(k, i).wait_recv()
            far = named_slots(far_ids[lane])[2]
            for d in range(experts):
                far_key[lane, d] = jnp.broadcast_to(far[d:d + 1], (8, n_tok))
            raw[lane] = normalized(raw[lane], far_sums[lane])

        def stage_p(k):
            lane, k = (0, k - 60) if k >= 60 else (1, k - 40)
            source = member((6, 4)[lane], 0)
            for j in peers(k):
                d = member(k, j)
                outgoing[far_slot(lane, d)] = picked(far_key[lane, d], raw.at[lane])
                dispatch(far_slot(lane, d), d, source).start()

        def stage_q(k):
            lane = 0 if k == 6 else 1
            rows[t, member(k, 0)] = picked(far_key[lane, e], raw.at[lane])

        def stage_a(k):
            local = k == 0 or k in relayed
            for j in range(1 if local else 0, size):
                s = member(k, j)
                dispatch(s, s, s).wait_recv()
            spread(rows, k, *row_sems)

        def shard_of(buf, k, n, psend, recv):
            if n is None or isinstance(n, int):
                n = n or 0
                shard = (partner + n_tp - 2 * n) % n_tp
                beside(buf, k, n, shard, psend, recv).wait_recv()
                return shard
            return n

        def taken(weights, shard, depth):
            return weights[pl.ds(pl.multiple_of(shard * depth, depth), depth), :]

        def gate_up(k, shards, gate=None, up=None):
            for n in shards:
                shard = shard_of(rows, k, n, rp_send, r_recv)
                part_rows = rows[shard, span(k)].reshape(size * cap, width)
                g = jnp.dot(part_rows, taken(wg, shard, width), preferred_element_type=F32)
                u = jnp.dot(part_rows, taken(wu, shard, width), preferred_element_type=F32)
                gate, up = (g, u) if gate is None else (gate + g, up + u)
            return gate, up

        def down(k, shards, made=None):
            units = hid.shape[3]
            for n in shards:
                shard = shard_of(hid, k, n, hp_send, h_recv)
                values = hid[shard, span(k)].reshape(size * cap, units)
                m = jnp.dot(values, taken(wd, shard, units), preferred_element_type=F32)
                made = m if made is None else made + m
            return made

        def stage_b(k):
            pass_on(rows, k, *row_sems)
            need(0, 1)
            near = [(t + n_tp - 2 * i) % n_tp for i in range(pairs)]
            gates[k], ups[k] = gate_up(k, near[:1] + [None] + near[1:])

        def stage_c(k):
            gate, up = gate_up(k, range(1, pairs), gates[k], ups[k])
            hidden = (gate / (1.0 + jnp.exp(-gate)) * up).astype(BF16)
            hid[t, span(k)] = hidden.reshape(size, cap, hidden.shape[1])
            spread(hid, k, *hid_sems)

        def stage_d(k):
            pass_on(hid, k, *hid_sems)
            need(2)
            near = [(t + n_tp - 2 * i) % n_tp for i in range(pairs)]
            mades[k] = down(k, near[:1] + [None] + near[1:])

        def stage_e(k):
            made = down(k, range(1, pairs), mades[k])
            prod[span(k)] = made.astype(BF16).reshape(size, cap, width)
            for j in peers(k):
                back(member(k, j), e).start()
            if k == 0:
                ret[e] = prod[e]

        def stage_f(k):
            for j in peers(k):
                d = member(k, j)
                back(d, d).wait_recv()
            base = (block ^ k) * size
            tables = jnp.concatenate(
                [chosen(key[base + j], weight[base + j][None]) for j in range(size)], axis=0)
            high = tables.astype(BF16)
            low = (tables - high.astype(F32)).astype(BF16)
            values = ret[span(k)].reshape(size * cap, width)
            dims = (((0,), (0,)), ((), ()))
            sums = lax.dot_general(high, values, dims, preferred_element_type=F32)
            sums = sums + lax.dot_general(low, values, dims, preferred_element_type=F32)
            if k != combined[0]:
                sums = sums + acc[...]
            if k != combined[-1]:
                acc[...] = sums
            else:
                out[...] = sums.astype(BF16)

        stages = dict(
            s=stage_s, o=stage_o, t=stage_t, w=stage_w, r=stage_r, p=stage_p, q=stage_q,
            a=stage_a, b=stage_b, c=stage_c, d=stage_d, e=stage_e, f=stage_f)
        for name, k in program:
            stages[name](k)

        for name, k in program:
            if name == "o":
                for j in peers(k):
                    d = member(k, j)
                    dispatch(own_slot(k, d), d, e).wait_send()
            if name == "p":
                lane, to = (0, k - 60) if k >= 60 else (1, k - 40)
                for j in peers(to):
                    d = member(to, j)
                    dispatch(far_slot(lane, d), d, e).wait_send()
            if name == "t":
                for i in range(3):
                    far_copy(k, i).wait_send()

    def steps(text):
        return [(item[0], int(item[1:])) for item in text]

    if relays:
        @pl.when(inner)
        def _():
            run(steps(INNER))

        @pl.when(jnp.logical_not(inner))
        def _():
            run(steps(OUTER))
    else:
        order = [("s", 0)] + [("o", k) for k in range(groups)]
        for k in range(groups):
            order += [(name, k) for name in "abcde"]
        run(order + [("f", k) for k in range(groups)])

    for i in range(1, n_tp):
        sq_copy(i, t).wait_send()
    for k in range(groups):
        for j in peers(k):
            back(member(k, j), e).wait_send()
        for buf, ysend, psend, recv in ((rows,) + row_sems, (hid,) + hid_sems):
            for i in range(pairs):
                if i > 0:
                    across(buf, k, i, t, ysend, recv).wait_send()
                beside(buf, k, i, t, psend, recv).wait_send()


def body(n_ep, n_tp, tokens, norm_gain, expert_ids, expert_weights, gate_weight, up_weight, down_weight):
    n_tok, width = tokens.shape
    experts = gate_weight.shape[0] * n_ep
    cap = 3 * n_tok * expert_ids.shape[1] // (2 * experts)
    depth, units = gate_weight.shape[1:]
    hidden = down_weight.shape[1]
    groups = next(g for g in (8, 4, 2, 1) if n_ep % g == 0)
    vmem = pl.BlockSpec(memory_space=pltpu.VMEM)
    hbm = pl.BlockSpec(memory_space=pl.ANY)
    dma = pltpu.SemaphoreType.DMA
    return pl.pallas_call(
        functools.partial(kernel, n_ep, n_tp, groups, cap),
        out_shape=pltpu.VMEM((n_tok, width), BF16),
        in_specs=[hbm] + [vmem] * 3 + [hbm] * 3,
        out_specs=vmem,
        scratch_shapes=[
            pltpu.VMEM((depth, units), BF16),
            pltpu.VMEM((depth, units), BF16),
            pltpu.VMEM((hidden, width), BF16),
            pltpu.VMEM((8, n_tok), F32),
            pltpu.VMEM((n_tp, 8, n_tok), F32),
            pltpu.VMEM((experts, 8, n_tok), F32),
            pltpu.VMEM((experts, 8, n_tok), F32),
            pltpu.VMEM((2 * n_ep, cap, width), BF16),
            pltpu.VMEM((n_tp, n_ep, cap, width), BF16),
            pltpu.VMEM((n_tp, n_ep, cap, units), BF16),
            pltpu.VMEM((n_ep, cap, width), BF16),
            pltpu.VMEM((n_ep, cap, width), BF16),
            pltpu.VMEM((n_tok, width), F32),
            pltpu.VMEM((n_tok, width), BF16),
            pltpu.VMEM((2, n_tok, width), BF16),
            pltpu.VMEM((8, n_tok), F32),
            pltpu.VMEM((2, 2, n_tok), jnp.int32),
            pltpu.VMEM((2, 8, n_tok), F32),
            pltpu.VMEM((2, experts, 8, n_tok), F32),
            pltpu.VMEM((n_tok, width), BF16),
            pltpu.VMEM((groups, n_ep // groups * cap, units), F32),
            pltpu.VMEM((groups, n_ep // groups * cap, units), F32),
            pltpu.VMEM((groups, n_ep // groups * cap, width), F32),
            dma((4,)), dma((n_tp,)), dma((n_tp,)), dma((2 * n_ep,)), dma((n_ep,)),
            dma((n_tp // 2, groups)), dma((n_tp // 2, groups)), dma((n_tp, groups)),
            dma((n_tp // 2, groups)), dma((n_tp // 2, groups)), dma((n_tp, groups)),
            dma((n_ep,)), dma((n_ep,)), dma((3,)), dma((2, 3)),
        ],
        compiler_params=pltpu.CompilerParams(
            collective_id=0, has_side_effects=True, vmem_limit_bytes=60 * 1024 * 1024),
    )(tokens, norm_gain[None, :], expert_ids.T, expert_weights.T, gate_weight, up_weight, down_weight)


def solution(mesh):
    in_specs = (
        P("ep", "tp"),
        P("tp"),
        P("ep", None),
        P("ep", None),
        P("ep", None, "tp"),
        P("ep", None, "tp"),
        P("ep", None, "tp"),
    )
    fn = functools.partial(body, mesh.shape["ep"], mesh.shape["tp"])
    return jax.shard_map(fn, mesh=mesh, in_specs=in_specs, out_specs=P("ep", "tp"), check_vma=False)
```
